256 devices in a mesh: ep: 64 (over z, y, core), tp: 4 (over x).
Axes of the slice: x: 4, y: 4, z: 8, core: 2. Of those that a mesh axis runs over, the one named last changes fastest.
Arguments:
- c_gate: bfloat16 [16384, 1024], P('ep', 'tp'), may hold values from -6 to 6
- b_gate: bfloat16 [16384, 1024], P('ep', 'tp'), may hold values from -6 to 6
- values: bfloat16 [16384, 1024], P('ep', 'tp'), may hold values from -6 to 6
- conv_taps: float32 [3, 1024], P(None, 'tp'), may hold values from -3.5 to 3.5
- w_mix_out: bfloat16 [1024, 2048], P('tp'), may hold values from -0.1875 to 0.1875
- moe_in: bfloat16 [32768, 2048], P(('ep', 'tp')), may hold values from -6 to 6
- norm_gain: float32 [2048], replicated, may hold values from 0.1 to 1.9
- route_ids: int32 [32768, 2], P(('ep', 'tp')), may hold values from 0 to 63, all different within a row; in each aligned block of 128 rows (0 to 127, 128 to 255, ...) at most 5 rows name the same one
- route_weights: float32 [32768, 2], P(('ep', 'tp')), may hold values from 0.1 to 1
- w_gate: bfloat16 [64, 2048, 3584], P('ep', None, 'tp'), may hold values from -0.125 to 0.125
- w_up: bfloat16 [64, 2048, 3584], P('ep', None, 'tp'), may hold values from -0.125 to 0.125
- w_down: bfloat16 [64, 3584, 2048], P('ep', 'tp'), may hold values from -0.09375 to 0.09375
Outputs:
- mixer_out: bfloat16 [16384, 2048], P(('ep', 'tp'))
- moe_out: bfloat16 [32768, 2048], P(('ep', 'tp'))
The draws below stay inside these ranges and needn't reach their ends.
Inputs may be any that keep to these rules, and one draw needn't show every extreme that they name: `route_ids`: each row names 2 different experts; in each aligned block of 128 rows (the rows of one device) no expert is named by more than 5 rows, and in every draw some expert is named by exactly 5 rows in some block.
All inputs are finite; a program needn't handle non-finite values.
Results may differ from the reference program's by a relative error of at most 0.012.
Values may be sent and summed in bfloat16 or wider, within the bound.
No kernel may reach another device: no remote copies, remote signals or barrier semaphores. Data moves between devices by JAX's collectives and lax.ppermute only.
A program may use at most 128 MiB of HBM per device.

```python
import math
import jax
import jax.numpy as jnp
import numpy as np
from jax import lax

D = 2048
WC = 1024
FF = 3584
KCONV = 3
TOP = 2
ROWS_B = 128
EXPERTS = 64
TOKA = 16384
TOKB = 32768
CAP = 5
SLOTS = 1280
N_EP = 64
N_TP = 4


def shard_levels(stream_key, shape, shards, smallest, largest):
    factor_of, own = 1.0, jax.random.fold_in(stream_key, 6)
    for axis_at, shards_of in shards:
        draws = jnp.exp(jax.random.uniform(jax.random.fold_in(own, axis_at), (shards_of,), jnp.float32, smallest / len(shards), largest / len(shards)))
        factor_of = factor_of * jnp.repeat(draws, shape[axis_at] // shards_of).reshape([-1 if axis == axis_at else 1 for axis in range(len(shape))])
    return factor_of


def shared_out(stream_key, own, number, rows, number_of, top, limit, lean):
    ranking = jax.random.permutation(stream_key, number_of)
    crowded, ordinary = shares(number_of, rows * top, limit, lean, True), shares(number_of, rows * top, limit, lean, False)
    places = jnp.arange(number_of)

    def named(lengths, offset_by):
        used = int((lengths > 0).sum())
        fixed = max(1, used // 4)
        passed = fixed + (places - fixed + offset_by * (used - fixed)) % max(1, number_of - fixed)
        return jnp.zeros((number_of,), jnp.int32).at[ranking[jnp.where(places < fixed, places, passed)]].set(jnp.asarray(lengths, jnp.int32))

    lengths = jnp.where(number % 4 == 0, named(crowded, number // 4), named(ordinary, number - number // 4 - 1))
    mixed = jax.random.permutation(jax.random.fold_in(own, 3), number_of)
    giver, sink = mixed[0:number_of // 2 * 2:2], mixed[1:number_of // 2 * 2:2]
    margin = jnp.minimum(lengths[giver] - 1, limit - lengths[sink]) // 2
    margin = jnp.where((giver == ranking[0]) | (sink == ranking[0]) | (lengths[sink] == 0), 0, jnp.maximum(margin, 0))
    passed = jax.random.randint(jax.random.fold_in(own, 4), (number_of // 2,), 0, 1 << 20) % (margin + 1)
    lengths = lengths.at[giver].add(-passed).at[sink].add(passed)
    labels = jnp.searchsorted(jnp.cumsum(lengths), jnp.arange(rows * top), side="right").astype(jnp.int32)
    grid = labels.reshape(top, rows).T
    grid = grid[jax.random.permutation(jax.random.fold_in(own, 1), rows)]
    offset_by = jax.random.randint(jax.random.fold_in(own, 2), (rows, 1), 0, top)
    return jnp.take_along_axis(grid, (jnp.arange(top)[None, :] + offset_by) % top, axis=1)


def shares(number_of, total, most, skew, full):
    weights = [(1 << 20) // math.isqrt(grade ** skew) + 1 for grade in range(1, number_of + 1)]
    largest = most if full else min(most, max(-(-total // number_of), total * weights[0] // sum(weights)))
    least = 1 if total - largest >= number_of - 1 else 0
    holding, rest = [largest] + [least] * (number_of - 1), total - largest - least * (number_of - 1)
    while rest > 0:
        candidates = [i for i in range(1, number_of) if holding[i] < largest] or [i for i in range(1, number_of) if holding[i] < most]
        pool, remaining = sum([weights[i] for i in candidates]), rest
        for i in candidates:
            extra = min(most - holding[i], max(1, remaining * weights[i] // pool), rest)
            holding[i] = holding[i] + extra
            rest = rest - extra
    return np.array(holding)


def gaussian(stream_key, shape, deviation, limit, split=(), kind=jnp.bfloat16):
    drawn = deviation * jax.random.normal(stream_key, shape, jnp.float32)
    if split:
        drawn = drawn * shard_levels(stream_key, shape, split, -0.22, 0.18)
    return jnp.clip(drawn, -limit, limit).astype(kind)


def setup_inputs(seed: int = 0) -> dict:
    streams_of = jax.random.split(jax.random.key(seed), 13)
    c_gate = gaussian(streams_of[0], (TOKA, WC), 1.0, 6.0, ((0, 64), (1, 4)))
    b_gate = gaussian(streams_of[1], (TOKA, WC), 1.0, 6.0, ((0, 64), (1, 4)))
    values = gaussian(streams_of[2], (TOKA, WC), 1.0, 6.0, ((0, 64), (1, 4)))
    conv_taps = gaussian(streams_of[3], (KCONV, WC), KCONV ** -0.5, 3.5, ((1, 4),), jnp.float32)
    w_mix_out = gaussian(streams_of[4], (WC, D), WC ** -0.5, 0.1875, ((0, 4),))
    moe_in = gaussian(streams_of[5], (TOKB, D), 1.0, 6.0, ((0, 256),))
    norm_gain = jnp.clip(1.0 + 0.18 * jax.random.normal(streams_of[6], (D,), jnp.float32), 0.1, 1.9)
    route_ids_keys = jax.random.split(jax.random.fold_in(streams_of[7], 1), TOKB // ROWS_B)
    route_ids_turns = jax.random.permutation(jax.random.fold_in(streams_of[7], 3), TOKB // ROWS_B)
    route_ids = jax.vmap(lambda own, number: shared_out(jax.random.fold_in(streams_of[7], 2), own, number, ROWS_B, EXPERTS, TOP, CAP, 1))(route_ids_keys, route_ids_turns).reshape((TOKB, TOP))
    route_weights = jnp.clip(0.1 + 0.9 * jax.random.uniform(streams_of[8], (TOKB, TOP), jnp.float32) ** shard_levels(streams_of[8], (TOKB, TOP), ((0, 256),), -0.2, 0.2), 0.1, 1.0)
    w_gate = gaussian(streams_of[9], (EXPERTS, D, FF), D ** -0.5, 0.125, ((0, 64), (2, 4)))
    w_up = gaussian(streams_of[10], (EXPERTS, D, FF), D ** -0.5, 0.125, ((0, 64), (2, 4)))
    w_down = gaussian(streams_of[11], (EXPERTS, FF, D), FF ** -0.5, 0.09375, ((0, 64), (1, 4)))
    return {"c_gate": c_gate, "b_gate": b_gate, "values": values, "conv_taps": conv_taps, "w_mix_out": w_mix_out, "moe_in": moe_in, "norm_gain": norm_gain, "route_ids": route_ids, "route_weights": route_weights, "w_gate": w_gate, "w_up": w_up, "w_down": w_down}


EPS = 1e-06

def grouped_product(left, right, groups):
    rows = left.shape[0]
    width = left.shape[1] // groups
    left_groups = left.reshape(rows, groups, width)
    right_groups = right.reshape(groups, width, right.shape[1])
    total = jnp.zeros((rows, right.shape[1]), jnp.float32)
    for group in range(groups):
        partial_value = jnp.dot(left_groups[:, group], right_groups[group], preferred_element_type=jnp.float32).astype(jnp.bfloat16)
        partial_value = lax.optimization_barrier(partial_value)
        total = total + partial_value.astype(jnp.float32)
    return total.astype(jnp.bfloat16)

def reference(c_gate, b_gate, values, conv_taps, w_mix_out, moe_in, norm_gain, route_ids, route_weights, w_gate, w_up, w_down):
    product = c_gate.astype(jnp.float32) * values.astype(jnp.float32)
    extended = jnp.concatenate([jnp.zeros((KCONV - 1, WC), jnp.float32), product], 0)
    convolved = jnp.zeros((TOKA, WC), jnp.float32)
    for offset in range(KCONV):
        convolved = convolved + conv_taps[offset][None, :] * extended[offset:offset + TOKA]
    mixed = (b_gate.astype(jnp.float32) * convolved).astype(jnp.bfloat16)
    mixer_out = grouped_product(mixed, w_mix_out, N_TP)
    stream = moe_in.astype(jnp.float32)
    scale = lax.rsqrt(lax.optimization_barrier(jnp.mean(stream * stream, axis=1, keepdims=True)) + EPS)
    normed = (stream * scale * norm_gain[None, :]).astype(jnp.bfloat16)
    copies = TOKB * TOP
    sources = N_EP * N_TP
    flat_ids = route_ids.reshape(sources, ROWS_B * TOP)
    onehot = (flat_ids[:, :, None] == jnp.arange(EXPERTS, dtype=jnp.int32)[None, None, :]).astype(jnp.int32)
    before = jnp.cumsum(onehot, axis=1) - onehot
    ranks_in = lax.optimization_barrier(jnp.sum(before * onehot, axis=2))
    slot_of = jnp.arange(sources, dtype=jnp.int32)[:, None] * CAP + ranks_in
    table = jnp.full((EXPERTS, SLOTS), copies, jnp.int32)
    table = table.at[flat_ids.reshape(-1), slot_of.reshape(-1)].set(jnp.arange(copies, dtype=jnp.int32))
    padded_rows = jnp.concatenate([normed, jnp.zeros((1, D), jnp.bfloat16)], 0)
    padded_weights = jnp.concatenate([route_weights.reshape(-1), jnp.zeros((1,), jnp.float32)], 0)

    def per_expert(carry, inputs):
        expert_table, gate_mat, up_mat, down_mat = inputs
        row_index = expert_table // TOP
        rows = padded_rows[row_index]
        gate_val = jnp.dot(rows, gate_mat, preferred_element_type=jnp.float32)
        up_val = jnp.dot(rows, up_mat, preferred_element_type=jnp.float32)
        hidden = (jax.nn.silu(gate_val) * up_val).astype(jnp.bfloat16)
        expert_out = grouped_product(hidden, down_mat, N_TP)
        weighted = expert_out.astype(jnp.float32) * padded_weights[expert_table][:, None]
        carry = carry.at[row_index].add(weighted, mode='drop')
        return (carry, None)
    summed, unused = lax.scan(per_expert, jnp.zeros((TOKB, D), jnp.float32), (table, w_gate, w_up, w_down))
    moe_out = summed.astype(jnp.bfloat16)
    return (mixer_out, moe_out)
```

```python
import jax
import jax.numpy as jnp
from jax import lax
from jax.experimental import pallas as pl
from jax.experimental.pallas import tpu as pltpu
from jax.sharding import PartitionSpec as P

EPS = 1e-06
CHUNKS = (1, 2, 2)
TOP = 2
LANES = 128


def ring(size, step):
    return [(i, (i + step) % size) for i in range(size)]


def shift(block, step):
    return lax.ppermute(block, "tp", ring(lax.axis_size("tp"), step))


def prep_kernel(ids_ref, stream_ref, gain_ref, *outs, experts, chunks):
    rows = stream_ref.shape[0]
    ids = ids_ref[...]
    expert = lax.broadcasted_iota(jnp.int32, (experts, rows), 0)
    picks = [(expert == ids[k : k + 1, :]).astype(jnp.float32) for k in range(TOP)]
    both = picks[0] + picks[1]
    earlier = lax.broadcasted_iota(jnp.int32, (rows, rows), 0) < lax.broadcasted_iota(
        jnp.int32, (rows, rows), 1
    )
    before = jnp.dot(
        both.astype(jnp.bfloat16),
        earlier.astype(jnp.bfloat16),
        preferred_element_type=jnp.float32,
    )
    ranks = [
        jnp.sum(before * pick, axis=0, keepdims=True).astype(jnp.int32) for pick in picks
    ]
    stream = stream_ref[...].astype(jnp.float32)
    scale = lax.rsqrt(jnp.mean(stream * stream, axis=1, keepdims=True) + EPS)
    normed = (stream * scale * gain_ref[...]).astype(jnp.bfloat16)
    first = 0
    for c, slots in enumerate(chunks):
        row = lax.broadcasted_iota(jnp.int32, (experts * slots, rows), 0)
        chosen = []
        for k in range(TOP):
            rank = ranks[k] - first
            inside = (rank >= 0) & (rank < slots)
            place = jnp.where(inside, ids[k : k + 1, :] * slots + rank, -1)
            chosen.append((row == place).astype(jnp.bfloat16))
        outs[2 * c][...] = jnp.dot(
            chosen[0] + chosen[1], normed, preferred_element_type=jnp.float32
        ).astype(jnp.bfloat16)
        outs[2 * c + 1][...] = jnp.concatenate(chosen, axis=1)
        first = first + slots


def prep(route_ids, moe_in, norm_gain, experts):
    rows, width = moe_in.shape
    shapes = []
    for slots in CHUNKS:
        shapes.append(jax.ShapeDtypeStruct((experts * slots, width), jnp.bfloat16))
        shapes.append(jax.ShapeDtypeStruct((experts * slots, TOP * rows), jnp.bfloat16))
    outs = pl.pallas_call(
        lambda *refs: prep_kernel(*refs, experts=experts, chunks=CHUNKS),
        out_shape=shapes,
        name="prep",
    )(route_ids.T, moe_in, norm_gain[None, :])
    return outs[0::2], outs[1::2]


def expert_kernel(*refs, count, pieces):
    xs = refs[:count]
    gate_ref, up_ref, down_ref = refs[count : count + 3]
    outs = refs[count + 3 : count + 3 + len(pieces)]
    rows_ref, acc_ref = refs[count + 3 + len(pieces) :]
    step = pl.program_id(0)

    @pl.when(step == 0)
    def _():
        at = 0
        for x in xs:
            rows_ref[at : at + x.shape[0], :] = x[...]
            at = at + x.shape[0]
        acc_ref[...] = jnp.zeros_like(acc_ref)

    rows = rows_ref[...]
    gate_val = jnp.dot(rows, gate_ref[0], preferred_element_type=jnp.float32)
    up_val = jnp.dot(rows, up_ref[0], preferred_element_type=jnp.float32)
    hidden = (gate_val / (1.0 + jnp.exp(-gate_val)) * up_val).astype(jnp.bfloat16)
    acc_ref[...] += jnp.dot(hidden, down_ref[0], preferred_element_type=jnp.float32)

    @pl.when(step == pl.num_programs(0) - 1)
    def _():
        at = 0
        for out in outs:
            out[...] = acc_ref[at : at + out.shape[0], :].astype(jnp.bfloat16)
            at = at + out.shape[0]


def expert(xs, pieces, w_gate, w_up, w_down, name):
    width, hidden = w_gate.shape[1:]
    block = 128 if hidden % 128 == 0 else hidden
    rows = sum(x.shape[0] for x in xs)
    whole = lambda shape: pl.BlockSpec(shape, lambda i: (0, 0))
    return pl.pallas_call(
        lambda *refs: expert_kernel(*refs, count=len(xs), pieces=pieces),
        grid=(hidden // block,),
        in_specs=[whole(x.shape) for x in xs]
        + [
            pl.BlockSpec((1, width, block), lambda i: (0, 0, i)),
            pl.BlockSpec((1, width, block), lambda i: (0, 0, i)),
            pl.BlockSpec((1, block, width), lambda i: (0, i, 0)),
        ],
        out_specs=[whole((n, width)) for n in pieces],
        out_shape=[jax.ShapeDtypeStruct((n, width), jnp.bfloat16) for n in pieces],
        scratch_shapes=[
            pltpu.VMEM((rows, width), jnp.bfloat16),
            pltpu.VMEM((rows, width), jnp.float32),
        ],
        cost_estimate=pl.CostEstimate(
            flops=6 * rows * width * hidden,
            bytes_accessed=6 * width * hidden + 4 * rows * width,
            transcendentals=rows * hidden,
        ),
        name=name,
    )(*xs, w_gate, w_up, w_down)


def finish_kernel(weights_ref, *refs, count):
    out_ref = refs[-1]
    rows = out_ref.shape[0]
    total = jnp.zeros(out_ref.shape, jnp.float32)
    for k in range(TOP):
        picked = jnp.zeros(out_ref.shape, jnp.float32)
        for c in range(count):
            picked = picked + lax.dot_general(
                refs[2 * c + 1][:, k * rows : (k + 1) * rows],
                refs[2 * c][...],
                (((0,), (0,)), ((), ())),
                preferred_element_type=jnp.float32,
            )
        total = total + picked * weights_ref[:, k : k + 1]
    out_ref[...] = total.astype(jnp.bfloat16)


def finish(route_weights, returned, chosen):
    rows = route_weights.shape[0]
    width = returned[0].shape[1]
    return pl.pallas_call(
        lambda *refs: finish_kernel(*refs, count=len(returned)),
        out_shape=jax.ShapeDtypeStruct((rows, width), jnp.bfloat16),
        name="finish",
    )(route_weights, *[x for pair in zip(returned, chosen) for x in pair])


def added(*blocks):
    return sum(block.astype(jnp.float32) for block in blocks).astype(jnp.bfloat16)


def exchanged(rows, slots):
    n_ep = lax.axis_size("ep")
    width = rows.shape[1]
    blocks = rows.reshape(n_ep, -1, LANES)
    moved = lax.all_to_all(blocks, "ep", split_axis=0, concat_axis=0, tiled=True)
    return moved.reshape(-1, width)


def mixer(c_gate, b_gate, values, conv_taps, w_mix_out):
    tokens = c_gate.shape[0]
    reach = conv_taps.shape[0] - 1
    product = c_gate.astype(jnp.float32) * values.astype(jnp.float32)
    n_ep = lax.axis_size("ep")
    route = [(i - 1, i) for i in range(1, n_ep)]
    previous = lax.ppermute(product[tokens - reach :], "ep", route)
    extended = jnp.concatenate([previous, product], 0)
    convolved = jnp.zeros_like(product)
    for offset in range(reach + 1):
        convolved = convolved + conv_taps[offset][None, :] * extended[offset : offset + tokens]
    mixed = (b_gate.astype(jnp.float32) * convolved).astype(jnp.bfloat16)
    partial = jnp.dot(mixed, w_mix_out, preferred_element_type=jnp.float32).astype(jnp.bfloat16)
    n_tp = lax.axis_size("tp")
    blocks = partial.reshape(n_tp, tokens // n_tp, -1)
    arrived = lax.all_to_all(blocks, "tp", split_axis=0, concat_axis=0, tiled=True)
    return arrived.astype(jnp.float32).sum(axis=0).astype(jnp.bfloat16)


def on_device(
    c_gate,
    b_gate,
    values,
    conv_taps,
    w_mix_out,
    moe_in,
    norm_gain,
    route_ids,
    route_weights,
    w_gate,
    w_up,
    w_down,
):
    experts = w_gate.shape[0] * lax.axis_size("ep")
    outgoing, chosen = prep(route_ids, moe_in, norm_gain, experts)
    arrived = [exchanged(rows, slots) for rows, slots in zip(outgoing, CHUNKS)]
    mixer_out = mixer(c_gate, b_gate, values, conv_taps, w_mix_out)
    returned = []
    for c, own in enumerate(arrived):
        n = own.shape[0]
        h = n // 2
        left = shift(own, 1)
        right = shift(own, -1)
        far_a = shift(left[:h], 1)
        far_b = shift(right[h:], -1)
        p_own, p_left, p_right_a, p_right_b = expert(
            (own, left, right), (n, n, h, h), w_gate, w_up, w_down, f"near{c}"
        )
        p_far_a, p_far_b = expert((far_a, far_b), (h, h), w_gate, w_up, w_down, f"far{c}")
        via_a = shift(p_far_a, 1)
        via_b = shift(p_far_b, -1)
        to_right = jnp.concatenate([added(p_right_a, via_a), p_right_b], 0)
        to_left = jnp.concatenate([p_left[:h], added(p_left[h:], via_b)], 0)
        from_left = shift(to_right, 1)
        from_right = shift(to_left, -1)
        total = added(p_own, from_left, from_right)
        returned.append(exchanged(total, CHUNKS[c]))
    moe_out = finish(route_weights, returned, chosen)
    return (mixer_out, moe_out)


def solution(mesh):
    return jax.shard_map(
        on_device,
        mesh=mesh,
        in_specs=(
            P("ep", "tp"),
            P("ep", "tp"),
            P("ep", "tp"),
            P(None, "tp"),
            P("tp", None),
            P(("ep", "tp"), None),
            P(),
            P(("ep", "tp"), None),
            P(("ep", "tp"), None),
            P("ep", None, "tp"),
            P("ep", None, "tp"),
            P("ep", "tp", None),
        ),
        out_specs=(P(("ep", "tp"), None), P(("ep", "tp"), None)),
        check_vma=False,
    )
```

```python
import jax
import jax.numpy as jnp
from jax import lax
from jax.experimental import pallas as pl
from jax.experimental.pallas import tpu as pltpu
from jax.sharding import PartitionSpec as P

EPS = 1e-06
CHUNKS = (2, 3)
TOP = 2
LANES = 128


def ring(size, step):
    return [(i, (i + step) % size) for i in range(size)]


def shift(block, step):
    return lax.ppermute(block, "tp", ring(lax.axis_size("tp"), step))


def to_lane_rows(scratch, value):
    groups = value.shape[1] // LANES
    rows = value.shape[0]
    for j in range(groups):
        scratch[pl.ds(j, rows, stride=groups), :] = value[:, j * LANES : (j + 1) * LANES]


def prep_kernel(ids_ref, stream_ref, gain_ref, *refs, experts, chunks):
    outs, scratch = refs[:-1], refs[-1]
    rows, _ = stream_ref.shape
    ids = ids_ref[...]
    expert = lax.broadcasted_iota(jnp.int32, (experts, rows), 0)
    picks = [(expert == ids[k : k + 1, :]).astype(jnp.float32) for k in range(TOP)]
    both = picks[0] + picks[1]
    earlier = lax.broadcasted_iota(jnp.int32, (rows, rows), 0) < lax.broadcasted_iota(
        jnp.int32, (rows, rows), 1
    )
    before = jnp.dot(
        both.astype(jnp.bfloat16),
        earlier.astype(jnp.bfloat16),
        preferred_element_type=jnp.float32,
    )
    ranks = [
        jnp.sum(before * pick, axis=0, keepdims=True).astype(jnp.int32) for pick in picks
    ]
    stream = stream_ref[...].astype(jnp.float32)
    scale = lax.rsqrt(jnp.mean(stream * stream, axis=1, keepdims=True) + EPS)
    normed = (stream * scale * gain_ref[...]).astype(jnp.bfloat16)
    total = sum(chunks)

    def selected(first, slots):
        row = lax.broadcasted_iota(jnp.int32, (experts * slots, rows), 0)
        found = []
        for k in range(TOP):
            rank = ranks[k] - first
            inside = (rank >= 0) & (rank < slots)
            place = jnp.where(inside, ids[k : k + 1, :] * slots + rank, -1)
            found.append((row == place).astype(jnp.bfloat16))
        return found

    found = selected(0, total)
    packed = jnp.dot(found[0] + found[1], normed, preferred_element_type=jnp.float32)
    to_lane_rows(scratch, packed)
    outs[0][...] = scratch[...].astype(jnp.bfloat16).reshape(outs[0].shape)
    first = 0
    for c, slots in enumerate(chunks):
        outs[1 + c][...] = jnp.concatenate(selected(first, slots), axis=1)
        first = first + slots


def prep(route_ids, moe_in, norm_gain, experts):
    rows, width = moe_in.shape
    groups = width // LANES
    total = sum(CHUNKS)
    shapes = [jax.ShapeDtypeStruct((experts, total * groups, LANES), jnp.bfloat16)]
    for slots in CHUNKS:
        shapes.append(jax.ShapeDtypeStruct((experts * slots, TOP * rows), jnp.bfloat16))
    outs = pl.pallas_call(
        lambda *refs: prep_kernel(*refs, experts=experts, chunks=CHUNKS),
        out_shape=shapes,
        scratch_shapes=[pltpu.VMEM((experts * total * groups, LANES), jnp.float32)],
        name="prep",
    )(route_ids.T, moe_in, norm_gain[None, :])
    return outs[0], outs[1:]


def unpack_kernel(in_ref, *refs, first, lanes):
    outs, scratch = refs[:-1], refs[-1]
    part = in_ref[:, first : first + lanes, :]
    scratch[...] = part.astype(jnp.float32).reshape(scratch.shape)
    at = 0
    for out in outs:
        rows, width = out.shape
        groups = width // LANES
        for j in range(groups):
            out[:, j * LANES : (j + 1) * LANES] = scratch[
                pl.ds(at * groups + j, rows, stride=groups), :
            ].astype(jnp.bfloat16)
        at = at + rows


def unpack(blocks, width, first, slots):
    groups = width // LANES
    half = blocks.shape[0] * slots // 2
    return pl.pallas_call(
        lambda *refs: unpack_kernel(*refs, first=first * groups, lanes=slots * groups),
        out_shape=[jax.ShapeDtypeStruct((half, width), jnp.bfloat16)] * 2,
        scratch_shapes=[pltpu.VMEM((2 * half * groups, LANES), jnp.float32)],
    )(blocks)


def merge_kernel(*refs):
    out, scratch = refs[-2:]
    parts = refs[:-2]
    per = len(parts) // 2
    at = 0
    for half in range(2):
        total = sum(ref[...].astype(jnp.float32) for ref in parts[half * per : (half + 1) * per])
        rows, width = total.shape
        groups = width // LANES
        for j in range(groups):
            scratch[pl.ds(at * groups + j, rows, stride=groups), :] = total[
                :, j * LANES : (j + 1) * LANES
            ]
        at = at + rows
    out[...] = scratch[...].astype(jnp.bfloat16).reshape(out.shape)


def merge(parts, experts):
    half, width = parts[0].shape
    lanes = 2 * half * width // LANES
    return pl.pallas_call(
        merge_kernel,
        out_shape=jax.ShapeDtypeStruct((experts, lanes // experts, LANES), jnp.bfloat16),
        scratch_shapes=[pltpu.VMEM((lanes, LANES), jnp.float32)],
    )(*parts)


def expert_kernel(*refs, count, cuts):
    xs = refs[:count]
    gate_hbm, up_hbm, down_hbm = refs[count : count + 3]
    outs = refs[count + 3 : 2 * count + 3]
    rows_v, gate_v, up_v, down_v, hidden_v, out_v = refs[2 * count + 3 : 2 * count + 9]
    x_sems, w_sems, o_sems = refs[2 * count + 9 :]
    n = xs[0].shape[0]
    waves = []
    for w, (at, size) in enumerate(cuts):
        cols = pl.ds(at, size)
        pair = []
        for i, (src, dst) in enumerate(((gate_hbm, gate_v), (up_hbm, up_v))):
            copy = pltpu.make_async_copy(src.at[0, :, cols], dst.at[:, cols], w_sems.at[2 * w + i])
            copy.start()
            pair.append(copy)
        waves.append(pair)
        if w == 0:
            loads = []
            for p, x in enumerate(xs):
                copy = pltpu.make_async_copy(x, rows_v.at[pl.ds(p * n, n), :], x_sems.at[p])
                copy.start()
                loads.append(copy)
    last = pltpu.make_async_copy(down_hbm.at[0], down_v, w_sems.at[2 * len(cuts)])
    last.start()
    for copy in loads:
        copy.wait()
    groups = 2 if count > 2 else 1
    per = count // groups
    group = per * n
    for (at, size), pair in zip(cuts, waves):
        for copy in pair:
            copy.wait()
        cols = pl.ds(at, size)

        def inner(i, carry, cols=cols):
            some = pl.ds(pl.multiple_of(i * group, group), group)
            rows = rows_v[some, :]
            gate_val = jnp.dot(rows, gate_v[:, cols], preferred_element_type=jnp.float32)
            up_val = jnp.dot(rows, up_v[:, cols], preferred_element_type=jnp.float32)
            hidden_v[some, cols] = (gate_val / (1.0 + jnp.exp(-gate_val)) * up_val).astype(
                jnp.bfloat16
            )
            return carry

        lax.fori_loop(0, groups, inner, 0)
    last.wait()

    stores = []
    for g in range(groups):
        some = pl.ds(g * group, group)
        out_v[some, :] = jnp.dot(
            hidden_v[some, :], down_v[...], preferred_element_type=jnp.float32
        ).astype(jnp.bfloat16)
        for q in range(g * per, (g + 1) * per):
            copy = pltpu.make_async_copy(out_v.at[pl.ds(q * n, n), :], outs[q], o_sems.at[q])
            copy.start()
            stores.append(copy)
    for copy in stores:
        copy.wait()


def expert(xs, w_gate, w_up, w_down):
    width, hidden = w_gate.shape[1:]
    n = xs[0].shape[0]
    count = len(xs)
    rows = n * count
    split = (hidden // 2 + 255) // 256 * 256
    cuts = ((0, split), (split, hidden - split))
    any_space = pl.BlockSpec(memory_space=pl.ANY)
    return pl.pallas_call(
        lambda *refs: expert_kernel(*refs, count=count, cuts=cuts),
        in_specs=[any_space] * (count + 3),
        out_specs=[any_space] * count,
        out_shape=[jax.ShapeDtypeStruct((n, width), jnp.bfloat16)] * count,
        scratch_shapes=[
            pltpu.VMEM((rows, width), jnp.bfloat16),
            pltpu.VMEM((width, hidden), jnp.bfloat16),
            pltpu.VMEM((width, hidden), jnp.bfloat16),
            pltpu.VMEM((hidden, width), jnp.bfloat16),
            pltpu.VMEM((rows, hidden), jnp.bfloat16),
            pltpu.VMEM((rows, width), jnp.bfloat16),
            pltpu.SemaphoreType.DMA((count,)),
            pltpu.SemaphoreType.DMA((2 * len(cuts) + 1,)),
            pltpu.SemaphoreType.DMA((count,)),
        ],
        cost_estimate=pl.CostEstimate(
            flops=6 * rows * width * hidden,
            bytes_accessed=6 * width * hidden + 4 * rows * width,
            transcendentals=rows * hidden,
        ),
    )(*xs, w_gate, w_up, w_down)


def picked_sum(weights_ref, blocks, chosen, scratch, rows_v):
    rows = weights_ref.shape[0]
    groups = rows_v.shape[1] // LANES
    scratch[...] = blocks[...].astype(jnp.float32).reshape(scratch.shape)
    for j in range(groups):
        rows_v[:, j * LANES : (j + 1) * LANES] = scratch[
            pl.ds(j, rows_v.shape[0], stride=groups), :
        ].astype(jnp.bfloat16)
    total = 0.0
    for k in range(TOP):
        picked = lax.dot_general(
            chosen[:, k * rows : (k + 1) * rows],
            rows_v[...],
            (((0,), (0,)), ((), ())),
            preferred_element_type=jnp.float32,
        )
        total = total + picked * weights_ref[:, k : k + 1]
    return total


def finish_kernel(weights_ref, blocks, chosen, *refs):
    out_ref, scratch, rows_v = refs[-3:]
    total = picked_sum(weights_ref, blocks, chosen, scratch, rows_v)
    for earlier in refs[:-3]:
        total = total + earlier[...]
    out_ref[...] = total.astype(out_ref.dtype)


def finish(route_weights, blocks, chosen, earlier, dtype):
    rows = route_weights.shape[0]
    copies = chosen.shape[0]
    lanes = blocks.shape[0] * blocks.shape[1]
    width = lanes * LANES // copies
    return pl.pallas_call(
        finish_kernel,
        out_shape=jax.ShapeDtypeStruct((rows, width), dtype),
        scratch_shapes=[
            pltpu.VMEM((lanes, LANES), jnp.float32),
            pltpu.VMEM((copies, width), jnp.bfloat16),
        ],
    )(route_weights, blocks, chosen, *earlier)


def added(*blocks):
    return sum(block.astype(jnp.float32) for block in blocks).astype(jnp.bfloat16)


def exchanged(blocks):
    return lax.all_to_all(blocks, "ep", split_axis=0, concat_axis=0, tiled=True)


def mixer(c_gate, b_gate, values, conv_taps, w_mix_out):
    tokens = c_gate.shape[0]
    reach = conv_taps.shape[0] - 1
    product = c_gate.astype(jnp.float32) * values.astype(jnp.float32)
    n_ep = lax.axis_size("ep")
    route = [(i - 1, i) for i in range(1, n_ep)]
    last = c_gate[tokens - reach :].astype(jnp.float32) * values[tokens - reach :].astype(jnp.float32)
    previous = lax.ppermute(last, "ep", route)
    extended = jnp.concatenate([previous, product], 0)
    convolved = jnp.zeros_like(product)
    for offset in range(reach + 1):
        convolved = convolved + conv_taps[offset][None, :] * extended[offset : offset + tokens]
    mixed = (b_gate.astype(jnp.float32) * convolved).astype(jnp.bfloat16)
    partial = jnp.dot(mixed, w_mix_out, preferred_element_type=jnp.float32).astype(jnp.bfloat16)
    n_tp = lax.axis_size("tp")
    here = lax.axis_index("tp")
    blocks = partial.reshape(n_tp, tokens // n_tp, -1)
    total = lax.dynamic_index_in_dim(blocks, here, 0, keepdims=False).astype(jnp.float32)
    for step in range(1, n_tp):
        block = lax.dynamic_index_in_dim(blocks, (here + step) % n_tp, 0, keepdims=False)
        total = total + shift(block, step).astype(jnp.float32)
    return total.astype(jnp.bfloat16)


def on_device(
    c_gate,
    b_gate,
    values,
    conv_taps,
    w_mix_out,
    moe_in,
    norm_gain,
    route_ids,
    route_weights,
    w_gate,
    w_up,
    w_down,
):
    experts = w_gate.shape[0] * lax.axis_size("ep")
    width = moe_in.shape[1]
    outgoing, chosen = prep(route_ids, moe_in, norm_gain, experts)
    mixer_out = mixer(c_gate, b_gate, values, conv_taps, w_mix_out)
    arrived = exchanged(outgoing)
    arrived, mixer_out = lax.optimization_barrier((arrived, mixer_out))
    returned = []
    first = 0
    for c, slots in enumerate(CHUNKS):
        own_a, own_b = unpack(arrived, width, first, slots)
        first = first + slots
        left_a, right_b = shift(own_a, 1), shift(own_b, -1)
        left_b, right_a = shift(own_b, 1), shift(own_a, -1)
        far_a, far_b = shift(left_a, 1), shift(right_b, -1)
        weights = (w_gate, w_up, w_down)
        pieces = (own_a, own_b, left_a, left_b, right_a, right_b)
        if c < len(CHUNKS) - 1:
            p = expert(pieces + (far_a, far_b), *weights)
        else:
            p = expert(pieces, *weights)
            p = list(p) + list(expert((far_a, far_b), *weights))
        via_a, via_b = shift(p[6], 1), shift(p[7], -1)
        from_left_b, from_right_a = shift(p[5], 1), shift(p[2], -1)
        from_left_a = shift(added(p[4], via_a), 1)
        from_right_b = shift(added(p[3], via_b), -1)
        parts = (p[0], from_left_a, from_right_a, p[1], from_left_b, from_right_b)
        merged = merge(parts, experts)
        returned.append(exchanged(merged))
    earlier = ()
    for c, (blocks, select) in enumerate(zip(returned, chosen)):
        kind = jnp.bfloat16 if c == len(CHUNKS) - 1 else jnp.float32
        earlier = (finish(route_weights, blocks, select, earlier, kind),)
    moe_out = earlier[0]
    return (mixer_out, moe_out)


def solution(mesh):
    return jax.shard_map(
        on_device,
        mesh=mesh,
        in_specs=(
            P("ep", "tp"),
            P("ep", "tp"),
            P("ep", "tp"),
            P(None, "tp"),
            P("tp", None),
            P(("ep", "tp"), None),
            P(),
            P(("ep", "tp"), None),
            P(("ep", "tp"), None),
            P("ep", None, "tp"),
            P("ep", None, "tp"),
            P("ep", "tp", None),
        ),
        out_specs=(P(("ep", "tp"), None), P(("ep", "tp"), None)),
        check_vma=False,
    )
```

```python
import jax
import jax.numpy as jnp
from jax import lax
from jax.experimental import pallas as pl
from jax.experimental.pallas import tpu as pltpu
from jax.sharding import PartitionSpec as P

EPS = 1e-06
CHUNKS = (2, 3)
TOP = 2
LANES = 128


def ring(size, step):
    return [(i, (i + step) % size) for i in range(size)]


def shift(block, step):
    return lax.ppermute(block, "tp", ring(lax.axis_size("tp"), step))


def widen(scratch, blocks, first, lanes):
    some = 8 * lanes

    def body(i, carry):
        part = blocks[pl.ds(i * 8, 8), first : first + lanes, :].astype(jnp.float32)
        scratch[pl.ds(pl.multiple_of(i * some, some), some), :] = part.reshape(some, LANES)
        return carry

    lax.fori_loop(0, blocks.shape[0] // 8, body, 0)


def narrow_to(blocks, scratch):
    lanes = blocks.shape[1]
    some = 8 * lanes

    def body(i, carry):
        part = scratch[pl.ds(pl.multiple_of(i * some, some), some), :].astype(jnp.bfloat16)
        blocks[pl.ds(i * 8, 8), :, :] = part.reshape(8, lanes, LANES)
        return carry

    lax.fori_loop(0, blocks.shape[0] // 8, body, 0)


def by_columns(width, body):
    def pair(i, carry):
        for j in range(2):
            body(2 * i + j, pl.ds(pl.multiple_of((2 * i + j) * LANES, LANES), LANES))
        return carry

    lax.fori_loop(0, width // LANES // 2, pair, 0)


def prep_kernel(ids_ref, stream_ref, gain_ref, out_ref, scratch, normed_v, *, experts, slots):
    rows, width = stream_ref.shape
    groups = width // LANES
    ids = ids_ref[...]
    expert = lax.broadcasted_iota(jnp.int32, (experts, rows), 0)
    picks = [(expert == ids[k : k + 1, :]).astype(jnp.float32) for k in range(TOP)]
    both = picks[0] + picks[1]
    earlier = lax.broadcasted_iota(jnp.int32, (rows, rows), 0) < lax.broadcasted_iota(
        jnp.int32, (rows, rows), 1
    )
    before = jnp.dot(
        both.astype(jnp.bfloat16),
        earlier.astype(jnp.bfloat16),
        preferred_element_type=jnp.float32,
    )
    stream = stream_ref[...].astype(jnp.float32)
    scale = lax.rsqrt(jnp.mean(stream * stream, axis=1, keepdims=True) + EPS)
    normed_v[...] = (stream * scale * gain_ref[...]).astype(jnp.bfloat16)
    row = lax.broadcasted_iota(jnp.int32, (experts * slots, rows), 0)
    found = 0.0
    for k in range(TOP):
        rank = jnp.sum(before * picks[k], axis=0, keepdims=True).astype(jnp.int32)
        place = ids[k : k + 1, :] * slots + rank
        found = found + (row == place).astype(jnp.bfloat16)

    def pack(i, carry):
        at = pl.ds(pl.multiple_of(i * 512, 512), 512)
        packed = jnp.dot(found, normed_v[:, at], preferred_element_type=jnp.float32)
        for j in range(512 // LANES):
            scratch[pl.ds(i * (512 // LANES) + j, experts * slots, stride=groups), :] = packed[
                :, j * LANES : (j + 1) * LANES
            ]
        return carry

    lax.fori_loop(0, width // 512, pack, 0)
    narrow_to(out_ref, scratch)


def prep(route_ids, moe_in, norm_gain, experts, slots):
    rows, width = moe_in.shape
    groups = width // LANES
    return pl.pallas_call(
        lambda *refs: prep_kernel(*refs, experts=experts, slots=slots),
        out_shape=jax.ShapeDtypeStruct((experts, slots * groups, LANES), jnp.bfloat16),
        scratch_shapes=[
            pltpu.VMEM((experts * slots * groups, LANES), jnp.float32),
            pltpu.VMEM((rows, width), jnp.bfloat16),
        ],
        name="prep",
    )(route_ids.T, moe_in, norm_gain[None, :])


def select_kernel(ids_ref, *outs, experts, chunks):
    rows = ids_ref.shape[0]
    ids = ids_ref[...]
    expert = lax.broadcasted_iota(jnp.int32, (rows, experts), 1)
    picks = [(expert == ids[:, k : k + 1]).astype(jnp.float32) for k in range(TOP)]
    both = picks[0] + picks[1]
    earlier = lax.broadcasted_iota(jnp.int32, (rows, rows), 0) > lax.broadcasted_iota(
        jnp.int32, (rows, rows), 1
    )
    before = jnp.dot(
        earlier.astype(jnp.bfloat16),
        both.astype(jnp.bfloat16),
        preferred_element_type=jnp.float32,
    )
    ranks = [
        jnp.sum(before * pick, axis=1, keepdims=True).astype(jnp.int32) for pick in picks
    ]
    first = 0
    for c, slots in enumerate(chunks):
        column = lax.broadcasted_iota(jnp.int32, (rows, experts * slots), 1)
        for k in range(TOP):
            rank = ranks[k] - first
            inside = (rank >= 0) & (rank < slots)
            place = jnp.where(inside, ids[:, k : k + 1] * slots + rank, -1)
            outs[c][k * rows : (k + 1) * rows, :] = (column == place).astype(jnp.bfloat16)
        first = first + slots


def select(route_ids, experts):
    rows = route_ids.shape[0]
    return pl.pallas_call(
        lambda *refs: select_kernel(*refs, experts=experts, chunks=CHUNKS),
        out_shape=[
            jax.ShapeDtypeStruct((TOP * rows, experts * slots), jnp.bfloat16) for slots in CHUNKS
        ],
        name="select",
    )(route_ids)


def unpack_kernel(in_ref, *refs, first, lanes):
    outs, scratch = refs[:-1], refs[-1]
    widen(scratch, in_ref, first, lanes)
    at = 0
    for out in outs:
        rows, width = out.shape
        groups = width // LANES

        def column(j, cols, out=out, at=at):
            part = scratch[pl.ds(at * groups + j, rows, stride=groups), :]
            out[:, cols] = part.astype(jnp.bfloat16)

        by_columns(width, column)
        at = at + rows


def unpack(blocks, width, first, slots):
    groups = width // LANES
    half = blocks.shape[0] * slots // 2
    return pl.pallas_call(
        lambda *refs: unpack_kernel(*refs, first=first * groups, lanes=slots * groups),
        out_shape=[jax.ShapeDtypeStruct((half, width), jnp.bfloat16)] * 2,
        scratch_shapes=[pltpu.VMEM((2 * half * groups, LANES), jnp.float32)],
    )(blocks)


def merge_kernel(*refs):
    out, scratch = refs[-2:]
    parts = refs[:-2]
    per = len(parts) // 2
    rows, width = parts[0].shape
    groups = width // LANES
    for half in range(2):

        def column(j, cols, half=half):
            total = sum(
                ref[:, cols].astype(jnp.float32) for ref in parts[half * per : (half + 1) * per]
            )
            scratch[pl.ds(half * rows * groups + j, rows, stride=groups), :] = total

        by_columns(width, column)
    narrow_to(out, scratch)


def merge(parts, experts):
    half, width = parts[0].shape
    lanes = 2 * half * width // LANES
    return pl.pallas_call(
        merge_kernel,
        out_shape=jax.ShapeDtypeStruct((experts, lanes // experts, LANES), jnp.bfloat16),
        scratch_shapes=[pltpu.VMEM((lanes, LANES), jnp.float32)],
    )(*parts)


def expert_kernel(*refs, count, pieces, cuts, columns):
    xs = refs[:count]
    gate_hbm, up_hbm, down_hbm = refs[count : count + 3]
    outs = refs[count + 3 : count + pieces + 3]
    rows_v, gate_v, up_v, down_v, hidden_v, out_v = refs[count + pieces + 3 : count + pieces + 9]
    x_sems, w_sems, o_sems = refs[count + pieces + 9 :]
    n = xs[0].shape[0]
    waves = []
    for w, (at, size) in enumerate(cuts):
        cols = pl.ds(at, size)
        pair = []
        for i, (src, dst) in enumerate(((gate_hbm, gate_v), (up_hbm, up_v))):
            copy = pltpu.make_async_copy(src.at[0, :, cols], dst.at[:, cols], w_sems.at[2 * w + i])
            copy.start()
            pair.append(copy)
        waves.append(pair)
        if w == 0:
            loads = []
            for p, x in enumerate(xs):
                copy = pltpu.make_async_copy(x, rows_v.at[pl.ds(p * n, n), :], x_sems.at[p])
                copy.start()
                loads.append(copy)
    last = pltpu.make_async_copy(down_hbm.at[0], down_v, w_sems.at[2 * len(cuts)])
    last.start()
    for copy in loads:
        copy.wait()
    groups = 2 if pieces > 2 else 1
    per = pieces // groups
    size_out = outs[0].shape[0]
    group = per * size_out
    for (at, size), pair in zip(cuts, waves):
        for copy in pair:
            copy.wait()
        cols = pl.ds(at, size)

        def inner(i, carry, cols=cols):
            some = pl.ds(pl.multiple_of(i * group, group), group)
            rows = rows_v[some, :]
            gate_val = jnp.dot(rows, gate_v[:, cols], preferred_element_type=jnp.float32)
            up_val = jnp.dot(rows, up_v[:, cols], preferred_element_type=jnp.float32)
            hidden_v[some, cols] = (gate_val / (1.0 + jnp.exp(-gate_val)) * up_val).astype(
                jnp.bfloat16
            )
            return carry

        lax.fori_loop(0, groups, inner, 0)
    last.wait()

    stores = []

    def store(first, last):
        for q in range(first, last):
            rows = pl.ds(q * size_out, size_out)
            copy = pltpu.make_async_copy(out_v.at[rows, :], outs[q], o_sems.at[q])
            copy.start()
            stores.append(copy)

    blocks = out_v.shape[1] // columns

    def outer(i, carry):
        some = pl.ds(pl.multiple_of(i // blocks * group, group), group)
        cols = pl.ds(pl.multiple_of(i % blocks * columns, columns), columns)
        out_v[some, cols] = jnp.dot(
            hidden_v[some, :], down_v[:, cols], preferred_element_type=jnp.float32
        ).astype(jnp.bfloat16)
        return carry

    lax.fori_loop(0, groups * blocks, outer, 0)
    store(0, pieces)
    for copy in stores:
        copy.wait()


def expert(xs, w_gate, w_up, w_down, columns):
    width, hidden = w_gate.shape[1:]
    n = xs[0].shape[0]
    count = len(xs)
    rows = n * count
    pieces = count
    split = (hidden // 2 + 255) // 256 * 256
    cuts = ((0, split), (split, hidden - split))
    any_space = pl.BlockSpec(memory_space=pl.ANY)
    return pl.pallas_call(
        lambda *refs: expert_kernel(*refs, count=count, pieces=pieces, cuts=cuts, columns=columns),
        in_specs=[any_space] * (count + 3),
        out_specs=[any_space] * pieces,
        out_shape=[jax.ShapeDtypeStruct((n, width), jnp.bfloat16)] * pieces,
        scratch_shapes=[
            pltpu.VMEM((rows, width), jnp.bfloat16),
            pltpu.VMEM((width, hidden), jnp.bfloat16),
            pltpu.VMEM((width, hidden), jnp.bfloat16),
            pltpu.VMEM((hidden, width), jnp.bfloat16),
            pltpu.VMEM((rows, hidden), jnp.bfloat16),
            pltpu.VMEM((rows, width), jnp.bfloat16),
            pltpu.SemaphoreType.DMA((count,)),
            pltpu.SemaphoreType.DMA((2 * len(cuts) + 1,)),
            pltpu.SemaphoreType.DMA((pieces,)),
        ],
        cost_estimate=pl.CostEstimate(
            flops=6 * rows * width * hidden,
            bytes_accessed=6 * width * hidden + 4 * rows * width,
            transcendentals=rows * hidden,
        ),
    )(*xs, w_gate, w_up, w_down)


def picked_sum(weights_ref, blocks, chosen, scratch, rows_v):
    rows = weights_ref.shape[0]
    groups = rows_v.shape[1] // LANES
    widen(scratch, blocks, 0, blocks.shape[1])

    def column(j, cols):
        part = scratch[pl.ds(j, rows_v.shape[0], stride=groups), :]
        rows_v[:, cols] = part.astype(jnp.bfloat16)

    by_columns(rows_v.shape[1], column)
    total = 0.0
    for k in range(TOP):
        picked = jnp.dot(
            chosen[k * rows : (k + 1) * rows, :],
            rows_v[...],
            preferred_element_type=jnp.float32,
        )
        total = total + picked * weights_ref[:, k : k + 1]
    return total


def finish_kernel(weights_ref, blocks, chosen, *refs):
    out_ref, scratch, rows_v = refs[-3:]
    total = picked_sum(weights_ref, blocks, chosen, scratch, rows_v)
    for earlier in refs[:-3]:
        total = total + earlier[...]
    out_ref[...] = total.astype(out_ref.dtype)


def finish(route_weights, blocks, chosen, earlier, dtype):
    rows = route_weights.shape[0]
    copies = chosen.shape[1]
    lanes = blocks.shape[0] * blocks.shape[1]
    width = lanes * LANES // copies
    return pl.pallas_call(
        finish_kernel,
        out_shape=jax.ShapeDtypeStruct((rows, width), dtype),
        scratch_shapes=[
            pltpu.VMEM((lanes, LANES), jnp.float32),
            pltpu.VMEM((copies, width), jnp.bfloat16),
        ],
    )(route_weights, blocks, chosen, *earlier)


def added(*blocks):
    return sum(block.astype(jnp.float32) for block in blocks).astype(jnp.bfloat16)


def exchanged(blocks):
    return lax.all_to_all(blocks, "ep", split_axis=0, concat_axis=0, tiled=True)


def mixer(c_gate, b_gate, values, conv_taps, w_mix_out):
    tokens = c_gate.shape[0]
    reach = conv_taps.shape[0] - 1
    product = c_gate.astype(jnp.float32) * values.astype(jnp.float32)
    n_ep = lax.axis_size("ep")
    route = [(i - 1, i) for i in range(1, n_ep)]
    last = c_gate[tokens - reach :].astype(jnp.float32) * values[tokens - reach :].astype(jnp.float32)
    previous = lax.ppermute(last, "ep", route)
    extended = jnp.concatenate([previous, product], 0)
    convolved = jnp.zeros_like(product)
    for offset in range(reach + 1):
        convolved = convolved + conv_taps[offset][None, :] * extended[offset : offset + tokens]
    mixed = (b_gate.astype(jnp.float32) * convolved).astype(jnp.bfloat16)
    partial = jnp.dot(mixed, w_mix_out, preferred_element_type=jnp.float32).astype(jnp.bfloat16)
    n_tp = lax.axis_size("tp")
    here = lax.axis_index("tp")
    blocks = partial.reshape(n_tp, tokens // n_tp, -1)
    arrived = [lax.dynamic_index_in_dim(blocks, here, 0, keepdims=False)]
    for step in range(1, n_tp):
        block = lax.dynamic_index_in_dim(blocks, (here + step) % n_tp, 0, keepdims=False)
        arrived.append(shift(block, step))
    return arrived


def on_device(
    c_gate,
    b_gate,
    values,
    conv_taps,
    w_mix_out,
    moe_in,
    norm_gain,
    route_ids,
    route_weights,
    w_gate,
    w_up,
    w_down,
):
    experts = w_gate.shape[0] * lax.axis_size("ep")
    rows, width = moe_in.shape
    slots = 5 * rows * TOP // (4 * experts)
    weights = (w_gate, w_up, w_down)
    outgoing = prep(route_ids, moe_in, norm_gain, experts, slots)
    mixed = mixer(c_gate, b_gate, values, conv_taps, w_mix_out)
    late_ids, outgoing = lax.optimization_barrier((route_ids, outgoing))
    chosen = select(late_ids, experts)
    arrived = exchanged(outgoing)
    returned = []
    first = 0
    for c, count in enumerate(CHUNKS):
        own_a, own_b = unpack(arrived, width, first, count)
        first = first + count
        left_a, right_b = shift(own_a, 1), shift(own_b, -1)
        left_b, right_a = shift(own_b, 1), shift(own_a, -1)
        far_a, far_b = shift(left_a, 1), shift(right_b, -1)
        close = (own_a, own_b, left_a, left_b, right_a, right_b)
        far = (far_a, far_b)
        if c < len(CHUNKS) - 1:
            p = expert(close + far, *weights, width // 2)
        else:
            p = expert(close, *weights, width)
            p = list(p) + list(expert(far, *weights, width))
        own_a, own_b, left_a, left_b, right_a, right_b, far_a, far_b = p
        via_a, via_b = shift(far_a, 1), shift(far_b, -1)
        from_left_b, from_right_a = shift(right_b, 1), shift(left_a, -1)
        from_left_a = shift(added(right_a, via_a), 1)
        from_right_b = shift(added(left_b, via_b), -1)
        parts = (own_a, from_left_a, from_right_a, own_b, from_left_b, from_right_b)
        merged = merge(parts, experts)
        returned.append(exchanged(merged))
    mixed, merged = lax.optimization_barrier((mixed, merged))
    mixer_out = added(*mixed)
    earlier = ()
    for c, (blocks, picks) in enumerate(zip(returned, chosen)):
        kind = jnp.bfloat16 if c == len(CHUNKS) - 1 else jnp.float32
        earlier = (finish(route_weights, blocks, picks, earlier, kind),)
    moe_out = earlier[0]
    return (mixer_out, moe_out)


def solution(mesh):
    return jax.shard_map(
        on_device,
        mesh=mesh,
        in_specs=(
            P("ep", "tp"),
            P("ep", "tp"),
            P("ep", "tp"),
            P(None, "tp"),
            P("tp", None),
            P(("ep", "tp"), None),
            P(),
            P(("ep", "tp"), None),
            P(("ep", "tp"), None),
            P("ep", None, "tp"),
            P("ep", None, "tp"),
            P("ep", "tp", None),
        ),
        out_specs=(P(("ep", "tp"), None), P(("ep", "tp"), None)),
        check_vma=False,
    )
```
